32 devices in a mesh: ep: 8 (over z, x), tp: 4 (over y, core).
Axes of the slice: x: 2, y: 2, z: 4, core: 2. Of those that a mesh axis runs over, the one named last changes fastest.
Arguments:
- queries: bfloat16 [1024, 1536], P('ep', 'tp'), may hold values from -400 to 400
- token_latents: bfloat16 [1024, 512], P('ep'), may hold values from -6 to 6
- key_rotary: bfloat16 [1024, 32], P('ep'), may hold values from -6 to 6
- latent_norm_gain: float32 [512], replicated, may hold values from 0.1 to 1.9
- latent_up_weight: bfloat16 [512, 2048], P(None, 'tp'), may hold values from -0.25 to 0.25
- w_out: bfloat16 [1024, 2048], P('tp'), may hold values from -0.1875 to 0.1875
- tokens_b: bfloat16 [1024, 2048], P('ep'), may hold values from -6 to 6
- moe_gain: float32 [2048], replicated, may hold values from 0.1 to 1.9
- group_logits: float32 [1024, 4], P('ep'), may hold values from -6 to 6
- inner_logits: float32 [1024, 2], P('ep'), may hold values from -6 to 6
- expert_pick: int32 [1024, 2], P('ep'), may hold values from 0 to 7, as said below
- w_gate: bfloat16 [8, 2048, 4096], P('ep', None, 'tp'), may hold values from -0.125 to 0.125
- w_up: bfloat16 [8, 2048, 4096], P('ep', None, 'tp'), may hold values from -0.125 to 0.125
- w_down: bfloat16 [8, 4096, 2048], P('ep', 'tp'), may hold values from -0.09375 to 0.09375
Outputs:
- mixer_out: bfloat16 [1024, 2048], P(('ep', 'tp'))
- expert_out: bfloat16 [1024, 2048], P('ep', 'tp')
The draws below stay inside these ranges and needn't reach their ends.
Inputs may be any that keep to these rules, and one draw needn't show every extreme that they name: `expert_pick`: each row names two different experts of one group, a group being 2 consecutive experts. Among the 128 rows of one index of ep no expert is named more than 64 times; in every draw some expert is named exactly 64 times by the rows of every index of ep.
All inputs are finite; a program needn't handle non-finite values.
Results may differ from the reference program's by a relative error of at most 0.018.
The reference program's roundings to bfloat16 on the way count: a program that leaves them out, or rounds other values in their place, can miss the bound.
Values may be sent and summed in bfloat16 or wider, within the bound.
A program may use at most 64 MiB of HBM per device.

```python
import jax
import jax.numpy as jnp
from jax import lax

D = 2048
HEAD_TOTAL = 16
PLAIN_HEAD_SIZE = 64
D_ROPE = 32
VALUE_HEAD_SIZE = 64
LATENT_WIDTH = 512
FF = 4096
GROUPS = 4
TOP = 2
SEGMENT = 64
TOK_B = 128
ATTENTION_TOKENS = 1024
TOKENS_B = 1024
EXPERTS = 8
EPG = 2
CAP = 64
HEADS_DEV = 4
WIDTH_DEV = 1024
N_TP = 4


def draw_queries(key, part):
    drawn = jax.random.normal(key, (ATTENTION_TOKENS, HEAD_TOTAL * (PLAIN_HEAD_SIZE + D_ROPE)), jnp.float32)
    return jnp.clip(drawn, -400.0, 400.0).astype(jnp.bfloat16)


def draw_expert_pick(key, part):
    per_group = EXPERTS // GROUPS
    block_count = TOKENS_B // TOK_B
    heavy_group = jax.random.randint(jax.random.fold_in(key, 1), (), 0, GROUPS)
    block_keys = jax.random.split(jax.random.fold_in(key, 2), block_count)

    def one_block(block_key):
        cut_key, perm_key, row_key = jax.random.split(block_key, 3)
        half_rows = TOK_B // 2
        cut_points = jnp.sort(jax.random.randint(cut_key, (GROUPS - 2,), 0, half_rows + 1))
        edge_list = jnp.concatenate([jnp.zeros((1,), jnp.int32), cut_points.astype(jnp.int32), jnp.full((1,), half_rows, jnp.int32)])
        others = edge_list[1:] - edge_list[:-1]
        group_rank = (jnp.arange(GROUPS, dtype=jnp.int32) - heavy_group - 1) % GROUPS
        group_loads = jnp.where(group_rank == GROUPS - 1, half_rows, others[jnp.minimum(group_rank, GROUPS - 2)])
        group_ends = jnp.cumsum(group_loads)
        position = jnp.arange(TOK_B, dtype=jnp.int32)
        group_index = jnp.sum((position[:, None] >= group_ends[None, :]).astype(jnp.int32), axis=1)
        inside = position - (group_ends - group_loads)[group_index]
        perm_scores = jax.random.randint(perm_key, (GROUPS, per_group), 0, 1 << 20) * per_group
        perm_scores = perm_scores + jnp.arange(per_group, dtype=jnp.int32)[None, :]
        perm_table = jnp.argsort(perm_scores, axis=1).astype(jnp.int32)
        first_pick = perm_table[group_index, inside % per_group]
        second_pick = perm_table[group_index, (inside + 1) % per_group]
        both_picks = jnp.stack([group_index * per_group + first_pick, group_index * per_group + second_pick], axis=1)
        return jax.random.permutation(row_key, both_picks, axis=0)
    return jax.vmap(one_block)(block_keys).reshape(TOKENS_B, 2).astype(jnp.int32)


def block_levels(stream_key, dims, cuts, smallest, high):
    def one(dim, parts):
        draws = jax.random.uniform(jax.random.fold_in(jax.random.fold_in(stream_key, 6), dim), (parts,), jnp.float32, smallest / len(cuts), high / len(cuts))
        return jnp.repeat(jnp.exp(draws), dims[dim] // parts).reshape((-1,) + (1,) * (len(dims) - dim - 1))

    level = one(*cuts[0])
    for cut in cuts[1:]:
        level = level * one(*cut)
    return level


def centred(key, extent, deviation, reach, shards=(), kind=jnp.bfloat16):
    entries = deviation * jax.random.normal(key, extent, jnp.float32)
    if shards:
        entries = entries * block_levels(key, extent, shards, -0.22, 0.18)
    return jnp.clip(entries, -reach, reach).astype(kind)


def setup_inputs(seed: int = 0) -> dict:
    splits = jax.random.split(jax.random.key(seed), 15)
    queries = draw_queries(jax.random.fold_in(splits[14], 71), 0)
    token_latents = centred(splits[1], (ATTENTION_TOKENS, LATENT_WIDTH), 1.0, 6.0, ((0, 8),))
    key_rotary = centred(splits[2], (ATTENTION_TOKENS, D_ROPE), 1.0, 6.0, ((0, 8),))
    latent_norm_gain = jnp.clip(1.0 + 0.18 * jax.random.normal(splits[3], (LATENT_WIDTH,), jnp.float32), 0.1, 1.9)
    latent_up_weight = centred(splits[4], (LATENT_WIDTH, HEAD_TOTAL * (PLAIN_HEAD_SIZE + VALUE_HEAD_SIZE)), LATENT_WIDTH ** -0.5, 0.25, ((1, 4),))
    w_out = centred(splits[5], (HEAD_TOTAL * VALUE_HEAD_SIZE, D), (HEAD_TOTAL * VALUE_HEAD_SIZE) ** -0.5, 0.1875, ((0, 4),))
    tokens_b = centred(splits[6], (TOKENS_B, D), 1.0, 6.0, ((0, 8),))
    moe_gain = jnp.clip(1.0 + 0.18 * jax.random.normal(splits[7], (D,), jnp.float32), 0.1, 1.9)
    group_logits = centred(splits[8], (TOKENS_B, GROUPS), 1.5, 6.0, ((0, 8),), jnp.float32)
    inner_logits = centred(splits[9], (TOKENS_B, TOP), 1.5, 6.0, ((0, 8),), jnp.float32)
    expert_pick = draw_expert_pick(jax.random.fold_in(splits[14], 71), 0)
    w_gate = centred(splits[11], (EXPERTS, D, FF), D ** -0.5, 0.125, ((0, 8), (2, 4)))
    w_up = centred(splits[12], (EXPERTS, D, FF), D ** -0.5, 0.125, ((0, 8), (2, 4)))
    w_down = centred(splits[13], (EXPERTS, FF, D), FF ** -0.5, 0.09375, ((0, 8), (1, 4)))
    return dict(queries=queries, token_latents=token_latents, key_rotary=key_rotary, latent_norm_gain=latent_norm_gain, latent_up_weight=latent_up_weight, w_out=w_out, tokens_b=tokens_b, moe_gain=moe_gain, group_logits=group_logits, inner_logits=inner_logits, expert_pick=expert_pick, w_gate=w_gate, w_up=w_up, w_down=w_down)


def rotate(values, positions):
    half_size = values.shape[-1] // 2
    frequency = jnp.power(10000.0, -jnp.arange(half_size, dtype=jnp.float32) * 2.0 / values.shape[-1])
    angles = positions[:, None] * frequency[None, :]
    if values.ndim == 3:
        angles = angles[:, None, :]
    cosine = jnp.cos(angles)
    sine_part = jnp.sin(angles)
    first_half = values[..., :half_size]
    second_half = values[..., half_size:]
    return jnp.concatenate([first_half * cosine - second_half * sine_part, second_half * cosine + first_half * sine_part], axis=-1)

def mixer(queries, token_latents, key_rotary, latent_norm_gain, latent_up_weight, w_out):
    length = queries.shape[0]
    positions = jnp.arange(length, dtype=jnp.float32)
    query_heads = queries.reshape(length, HEAD_TOTAL, PLAIN_HEAD_SIZE + D_ROPE)
    q_plain = query_heads[:, :, :PLAIN_HEAD_SIZE]
    q_turned = rotate(query_heads[:, :, PLAIN_HEAD_SIZE:].astype(jnp.float32), positions).astype(jnp.bfloat16)
    latent = token_latents.astype(jnp.float32)
    normed_latent = (latent * lax.rsqrt(lax.optimization_barrier(jnp.mean(latent * latent, axis=-1, keepdims=True)) + 1e-06) * latent_norm_gain).astype(jnp.bfloat16)
    key_value = jnp.dot(normed_latent, latent_up_weight, preferred_element_type=jnp.float32).astype(jnp.bfloat16)
    key_value = key_value.reshape(length, HEAD_TOTAL, PLAIN_HEAD_SIZE + VALUE_HEAD_SIZE)
    k_turned = rotate(key_rotary.astype(jnp.float32), positions).astype(jnp.bfloat16)
    block_rows = 512 if length % 512 == 0 else length
    blocks = length // block_rows
    segment_all = jnp.arange(length, dtype=jnp.int32) // SEGMENT
    scale_factor = (PLAIN_HEAD_SIZE + D_ROPE) ** (-0.5)

    def one_head(head_args):
        plain_h, turned_h, key_h, value_h = head_args

        def one_block(block_args):
            plain_b, turned_b, first_row = block_args
            scores = jnp.dot(plain_b, key_h.T, preferred_element_type=jnp.float32)
            scores = scores + jnp.dot(turned_b, k_turned.T, preferred_element_type=jnp.float32)
            scores = scores * scale_factor
            query_segment = (first_row + jnp.arange(block_rows, dtype=jnp.int32)) // SEGMENT
            allowed = query_segment[:, None] >= segment_all[None, :]
            scores = jnp.where(allowed, scores, -jnp.inf)
            row_max = lax.optimization_barrier(jnp.max(scores, axis=-1, keepdims=True))
            exp_scores = jnp.exp(scores - row_max)
            denominator = lax.optimization_barrier(jnp.sum(exp_scores, axis=-1, keepdims=True))
            numerator = jnp.dot(exp_scores.astype(jnp.bfloat16), value_h, preferred_element_type=jnp.float32)
            return (numerator / denominator).astype(jnp.bfloat16)
        starts = jnp.arange(blocks, dtype=jnp.int32) * block_rows
        result = lax.map(one_block, (plain_h.reshape(blocks, block_rows, PLAIN_HEAD_SIZE), turned_h.reshape(blocks, block_rows, D_ROPE), starts))
        return result.reshape(length, VALUE_HEAD_SIZE)
    heads_out = lax.map(one_head, (q_plain.transpose(1, 0, 2), q_turned.transpose(1, 0, 2), key_value[:, :, :PLAIN_HEAD_SIZE].transpose(1, 0, 2), key_value[:, :, PLAIN_HEAD_SIZE:].transpose(1, 0, 2)))
    attended = heads_out.transpose(1, 0, 2).reshape(length, HEAD_TOTAL * VALUE_HEAD_SIZE)
    group_cols = HEADS_DEV * VALUE_HEAD_SIZE

    def add_group(group_index, running):
        first_col = (group_index * group_cols).astype(jnp.int32)
        columns = lax.dynamic_slice_in_dim(attended, first_col, group_cols, 1)
        weight_rows = lax.dynamic_slice_in_dim(w_out, first_col, group_cols, 0)
        partial_value = jnp.dot(columns, weight_rows, preferred_element_type=jnp.float32).astype(jnp.bfloat16)
        partial_value = lax.optimization_barrier(partial_value)
        return running + partial_value.astype(jnp.float32)
    total = lax.fori_loop(0, N_TP, add_group, jnp.zeros((length, D), jnp.float32))
    return total.astype(jnp.bfloat16)

def experts_half(tokens_b, moe_gain, group_logits, inner_logits, expert_pick, w_gate, w_up, w_down):
    total_rows = tokens_b.shape[0]
    values_f = tokens_b.astype(jnp.float32)
    centered = values_f - lax.optimization_barrier(jnp.mean(values_f, axis=-1, keepdims=True))
    variance = lax.optimization_barrier(jnp.mean(centered * centered, axis=-1, keepdims=True))
    normed = (centered * lax.rsqrt(variance + 1e-05) * moe_gain).astype(jnp.bfloat16)
    home_group = expert_pick[:, 0] // EPG
    own_logit = lax.optimization_barrier(jnp.sum(jnp.where(jnp.arange(GROUPS, dtype=jnp.int32)[None, :] == home_group[:, None], group_logits, 0.0), axis=1))
    group_share = 1.0 / lax.optimization_barrier(jnp.sum(jnp.exp(group_logits - own_logit[:, None]), axis=1))
    logit_gap = inner_logits[:, 0] - inner_logits[:, 1]
    route_weight = group_share[:, None] * jnp.stack([jax.nn.sigmoid(logit_gap), jax.nn.sigmoid(-logit_gap)], axis=1)
    slots_all = EXPERTS * CAP

    def one_expert(expert_id, running):
        matches = expert_pick == expert_id.astype(jnp.int32)
        named = jnp.any(matches, axis=1)
        picked_rows = jnp.nonzero(named, size=slots_all, fill_value=0)[0].astype(jnp.int32)
        live = jnp.arange(slots_all, dtype=jnp.int32) < jnp.sum(named.astype(jnp.int32))
        inputs = normed[picked_rows]
        gate_proj = jnp.dot(inputs, w_gate[expert_id], preferred_element_type=jnp.float32)
        up_proj = jnp.dot(inputs, w_up[expert_id], preferred_element_type=jnp.float32)
        hidden = (jax.nn.silu(gate_proj) * up_proj).astype(jnp.bfloat16)
        pieces = hidden.reshape(slots_all, N_TP, WIDTH_DEV).astype(jnp.float32)
        down_parts = w_down[expert_id].reshape(N_TP, WIDTH_DEV, D).astype(jnp.float32)
        partial_value = jnp.einsum('ntf,tfd->ntd', pieces, down_parts).astype(jnp.bfloat16)
        partial_value = lax.optimization_barrier(partial_value)
        result = lax.optimization_barrier(jnp.sum(partial_value.astype(jnp.float32), axis=1)).astype(jnp.bfloat16)
        result = lax.optimization_barrier(result)
        weight = lax.optimization_barrier(jnp.sum(jnp.where(matches[picked_rows], route_weight[picked_rows], 0.0), axis=1))
        weight = jnp.where(live, weight, 0.0)
        return running.at[picked_rows].add(weight[:, None] * result.astype(jnp.float32))
    total = lax.fori_loop(0, EXPERTS, one_expert, jnp.zeros((total_rows, D), jnp.float32))
    return total.astype(jnp.bfloat16)

def reference(queries, token_latents, key_rotary, latent_norm_gain, latent_up_weight, w_out, tokens_b, moe_gain, group_logits, inner_logits, expert_pick, w_gate, w_up, w_down):
    mixer_out = mixer(queries, token_latents, key_rotary, latent_norm_gain, latent_up_weight, w_out)
    expert_out = experts_half(tokens_b, moe_gain, group_logits, inner_logits, expert_pick, w_gate, w_up, w_down)
    return (mixer_out, expert_out)
```

```python
import functools

import jax
import jax.numpy as jnp
from jax import lax
from jax.experimental import pallas as pl
from jax.experimental.pallas import tpu as pltpu
from jax.sharding import PartitionSpec as P

PLAIN_HEAD_SIZE = 64
D_ROPE = 32
VALUE_HEAD_SIZE = 64
SEGMENT = 64


def rotate(values, positions):
    half_size = values.shape[-1] // 2
    frequency = jnp.power(
        10000.0, -jnp.arange(half_size, dtype=jnp.float32) * 2.0 / values.shape[-1]
    )
    angles = positions[:, None] * frequency[None, :]
    if values.ndim == 3:
        angles = angles[:, None, :]
    cosine = jnp.cos(angles)
    sine_part = jnp.sin(angles)
    first_half = values[..., :half_size]
    second_half = values[..., half_size:]
    return jnp.concatenate(
        [
            first_half * cosine - second_half * sine_part,
            second_half * cosine + first_half * sine_part,
        ],
        axis=-1,
    )


def finish_expert(gate_proj, up_proj, w_down, source_count, item_count, model_width):
    hidden = (jax.nn.silu(gate_proj) * up_proj).astype(jnp.bfloat16)
    partial_value = jnp.dot(hidden, w_down[0], preferred_element_type=jnp.float32)
    partial_value = partial_value.reshape(source_count, item_count, model_width)
    return lax.psum_scatter(
        partial_value.astype(jnp.bfloat16), "tp", scatter_dimension=2, tiled=True
    )


def per_device(
    queries,
    token_latents,
    key_rotary,
    latent_norm_gain,
    latent_up_weight,
    w_out,
    tokens_b,
    moe_gain,
    group_logits,
    inner_logits,
    expert_pick,
    w_gate,
    w_up,
    w_down,
):
    row_count = queries.shape[0]
    heads_here = w_out.shape[0] // VALUE_HEAD_SIZE
    offset = lax.axis_index("ep") * row_count
    token_index = offset + jnp.arange(row_count, dtype=jnp.int32)
    positions = token_index.astype(jnp.float32)
    query_heads = queries.reshape(row_count, heads_here, PLAIN_HEAD_SIZE + D_ROPE)
    q_plain = jnp.transpose(query_heads[:, :, :PLAIN_HEAD_SIZE], (1, 0, 2))
    q_turned = rotate(query_heads[:, :, PLAIN_HEAD_SIZE:].astype(jnp.float32), positions).astype(
        jnp.bfloat16
    )
    q_turned = jnp.transpose(q_turned, (1, 0, 2))
    latent = token_latents.astype(jnp.float32)
    normed_latent = (
        latent
        * lax.rsqrt(jnp.mean(latent * latent, axis=-1, keepdims=True) + 1e-06)
        * latent_norm_gain
    ).astype(jnp.bfloat16)
    k_turned = rotate(key_rotary.astype(jnp.float32), positions).astype(jnp.bfloat16)
    query_segment = token_index // SEGMENT
    scale_factor = (PLAIN_HEAD_SIZE + D_ROPE) ** (-0.5)
    own_keys = jnp.dot(normed_latent, latent_up_weight, preferred_element_type=jnp.float32).astype(
        jnp.bfloat16
    )
    shard_part = (
        lax.all_gather(own_keys, "ep", axis=0, tiled=True),
        lax.all_gather(k_turned, "ep", axis=0, tiled=True),
    )
    projected = shard_part[0].reshape(
        shard_part[0].shape[0], heads_here, PLAIN_HEAD_SIZE + VALUE_HEAD_SIZE
    )
    kv_heads = jnp.transpose(projected, (1, 0, 2))
    run_max = jnp.full((heads_here, row_count), -1e30, jnp.float32)
    key_count = kv_heads.shape[1]
    k_plain = kv_heads[:, :, :PLAIN_HEAD_SIZE]
    values = kv_heads[:, :, PLAIN_HEAD_SIZE:]
    scores = jnp.einsum("hqd,hkd->hqk", q_plain, k_plain, preferred_element_type=jnp.float32)
    scores = scores + jnp.einsum(
        "hqd,kd->hqk", q_turned, shard_part[1], preferred_element_type=jnp.float32
    )
    scores = scores * scale_factor
    key_segment = jnp.arange(key_count, dtype=jnp.int32) // SEGMENT
    allowed = query_segment[:, None] >= key_segment[None, :]
    scores = jnp.where(allowed[None], scores, -jnp.inf)
    new_max = jnp.maximum(run_max, jnp.max(scores, axis=-1))
    weights_raw = jnp.exp(scores - new_max[:, :, None])
    denominator = jnp.sum(weights_raw, axis=-1)
    update = jnp.einsum(
        "hqk,hkd->hqd", weights_raw.astype(jnp.bfloat16), values, preferred_element_type=jnp.float32
    )
    finished = (new_max, denominator, update)
    denominator = finished[1]
    attended = (finished[2] / denominator[:, :, None]).astype(jnp.bfloat16)
    attended = jnp.transpose(attended, (1, 0, 2)).reshape(row_count, heads_here * VALUE_HEAD_SIZE)
    mixer_out = lax.psum_scatter(
        jnp.dot(attended, w_out, preferred_element_type=jnp.float32).astype(jnp.bfloat16),
        "tp",
        scatter_dimension=0,
        tiled=True,
    )
    row_total = tokens_b.shape[0]
    model_width = tokens_b.shape[1]
    experts = lax.axis_size("ep")
    capacity = 4 * row_total // experts
    values_f = tokens_b.astype(jnp.float32)
    centered = values_f - jnp.mean(values_f, axis=-1, keepdims=True)
    variance = jnp.mean(centered * centered, axis=-1, keepdims=True)
    normed = (centered * lax.rsqrt(variance + 1e-05) * moe_gain).astype(jnp.bfloat16)
    flat_picks = expert_pick.reshape(-1)
    owner_row = jnp.arange(2 * row_total, dtype=jnp.int32) // 2
    hit_table = (flat_picks[:, None] == jnp.arange(experts, dtype=jnp.int32)[None, :]).astype(
        jnp.int32
    )
    order_in = jnp.sum(jnp.cumsum(hit_table, axis=0) * hit_table, axis=1) - 1
    slot_index = flat_picks * capacity + order_in
    slot_rows = jnp.zeros((experts * capacity,), jnp.int32).at[slot_index].set(owner_row)
    slot_filled = jnp.zeros((experts * capacity,), jnp.bfloat16).at[slot_index].set(1.0)
    outbound = (normed[slot_rows] * slot_filled[:, None]).reshape(experts, capacity, model_width)
    arrived = lax.all_to_all(outbound, "ep", split_axis=0, concat_axis=0, tiled=True)
    source_count = arrived.shape[0]
    item_count = arrived.shape[1]
    flat_rows = arrived.reshape(source_count * item_count, model_width)
    gate_proj = jnp.dot(flat_rows, w_gate[0], preferred_element_type=jnp.float32)
    up_proj = jnp.dot(flat_rows, w_up[0], preferred_element_type=jnp.float32)
    computed = finish_expert(gate_proj, up_proj, w_down, source_count, item_count, model_width)
    returned = lax.all_to_all(computed, "ep", split_axis=0, concat_axis=0, tiled=True)
    flat_back = returned.reshape(experts * capacity, returned.shape[2])
    chosen = flat_back[slot_index].astype(jnp.float32).reshape(row_total, 2, returned.shape[2])
    per_group = experts // group_logits.shape[1]
    home_group = expert_pick[:, 0] // per_group
    own_logit = jnp.sum(
        jnp.where(
            jnp.arange(group_logits.shape[1], dtype=jnp.int32)[None, :] == home_group[:, None],
            group_logits,
            0.0,
        ),
        axis=1,
    )
    group_share = 1.0 / jnp.sum(jnp.exp(group_logits - own_logit[:, None]), axis=1)
    logit_gap = inner_logits[:, 0] - inner_logits[:, 1]
    route_weight = group_share[:, None] * jnp.stack(
        [jax.nn.sigmoid(logit_gap), jax.nn.sigmoid(-logit_gap)], axis=1
    )
    expert_out = jnp.sum(route_weight[:, :, None] * chosen, axis=1).astype(jnp.bfloat16)
    return (mixer_out, expert_out)


MESH = pl.DeviceIdType.MESH
BF = jnp.bfloat16
F32 = jnp.float32


def dot(a, b):
    return jnp.dot(a, b, preferred_element_type=F32)


def fused_kernel(
    n_z,
    n_x,
    q_ref,
    lat_ref,
    kr_ref,
    lgain_ref,
    tok_ref,
    mgain_ref,
    glog_ref,
    ilog_ref,
    pick_ref,
    cos_ref,
    sin_ref,
    upw_hbm,
    wout_hbm,
    wg_hbm,
    wu_hbm,
    wd_hbm,
    mix_ref,
    exp_ref,
    upw,
    wout,
    wg,
    wu,
    wd,
    nrm,
    dsend,
    xb,
    gate,
    up,
    hidden,
    pa,
    ra,
    pb,
    rb,
    pc,
    rc,
    po,
    rsend,
    ret,
    kv,
    qt,
    att,
    mpart,
    mrecv,
    w_sem,
    z_sem,
    x_sem,
    y_sem,
    c_sem,
    f_sem,
    p_sem,
    rb_sem,
    ret_sem,
    kz_sem,
    kx_sem,
    m_sem,
):
    ep = lax.axis_index("ep")
    tp = lax.axis_index("tp")
    z, x = ep // n_x, lax.rem(ep, n_x)
    y, c = tp // 2, lax.rem(tp, 2)
    ox = 1 - x
    rows = tok_ref.shape[0]
    cap = dsend.shape[1]
    width = dsend.shape[2]
    heads = qt.shape[1] // 128
    other_x = (z * n_x + ox, tp)
    core = tp + 1 - 2 * c
    over = tp + 2 - 4 * y
    diag = 3 - tp
    to_core, to_y = (ep, core), (ep, over)

    loads = []
    for i, (a, b) in enumerate(
        ((upw_hbm, upw), (wg_hbm.at[0], wg), (wu_hbm.at[0], wu), (wd_hbm.at[0], wd), (wout_hbm, wout))
    ):
        cp = pltpu.make_async_copy(a, b, w_sem.at[i])
        cp.start()
        loads.append(cp)

    barrier = pltpu.get_barrier_semaphore()
    n_ep = n_z * n_x
    for d in range(1, n_ep):
        pl.semaphore_signal(
            barrier, inc=1, device_id=(lax.rem(ep + d, n_ep), tp), device_id_type=MESH
        )
    for d in range(1, 4):
        pl.semaphore_signal(
            barrier, inc=1, device_id=(ep, lax.rem(tp + d, 4)), device_id_type=MESH
        )

    pending = []

    def send(src, dst, sem, device):
        cp = pltpu.make_async_remote_copy(
            src_ref=src,
            dst_ref=dst,
            send_sem=sem.at[0],
            recv_sem=sem.at[1],
            device_id=device,
            device_id_type=MESH,
        )
        cp.start()
        pending.append(cp)
        return cp

    values_f = tok_ref[...].astype(F32)
    centered = values_f - jnp.mean(values_f, axis=-1, keepdims=True)
    variance = jnp.mean(centered * centered, axis=-1, keepdims=True)
    nrm[...] = (centered * lax.rsqrt(variance + 1e-05) * mgain_ref[...]).astype(BF)
    mine = nrm[:, pl.ds(pl.multiple_of(tp * width, width), width)]
    pick0 = pick_ref[:, 0:1]
    pick1 = pick_ref[:, 1:2]
    group = pick0 // n_x
    group_one = (lax.broadcasted_iota(jnp.int32, (rows, 128), 1) == group).astype(F32)
    below = (
        lax.broadcasted_iota(jnp.int32, (rows, rows), 0)
        > lax.broadcasted_iota(jnp.int32, (rows, rows), 1)
    ).astype(F32)
    counts = dot(below.astype(BF), group_one.astype(BF))
    order_in = jnp.sum(counts * group_one, axis=1, keepdims=True)
    slot = group.astype(F32) * float(cap) + order_in
    slot_iota = lax.broadcasted_iota(jnp.int32, (rows, n_z * cap), 1).astype(F32)
    table = (slot_iota == slot).astype(F32)
    picked = dot(table.T.astype(BF), mine).astype(BF)
    dsend[...] = picked.reshape(n_z, cap, width)
    xb[tp, z, x] = dsend[z]

    pl.semaphore_wait(barrier, n_ep + 2)

    z_in = [None]
    for d in range(1, n_z):
        far = lax.rem(z + d, n_z)
        z_in.append(send(dsend.at[far], xb.at[tp, z, x], z_sem.at[d], (far * n_x + x, tp)))

    def block(d):
        return lax.rem(z + n_z - d, n_z)

    x_in, y_in, c_in = [], [], []

    def relay_tp(d, side, xi):
        ref = xb.at[tp, block(d), xi]
        y_in.append(send(ref, ref, y_sem.at[d, side], to_y))
        c_in.append(send(ref, ref, c_sem.at[d, side], to_core))

    ref = xb.at[tp, z, x]
    x_in.append(send(dsend.at[z], ref, x_sem.at[0], other_x))
    relay_tp(0, 0, x)

    latent = lat_ref[...].astype(F32)
    normed_latent = (
        latent
        * lax.rsqrt(jnp.mean(latent * latent, axis=-1, keepdims=True) + 1e-06)
        * lgain_ref[...]
    ).astype(BF)
    cosine, sine_part = cos_ref[...], sin_ref[...]
    half = D_ROPE // 2
    head_size = PLAIN_HEAD_SIZE + D_ROPE

    def turn(values, n_heads, base, stride):
        wide = n_heads * 128
        src = lax.broadcasted_iota(jnp.int32, (values.shape[1], wide), 0)
        lane = lax.broadcasted_iota(jnp.int32, (values.shape[1], wide), 1)
        t = lax.rem(lane, 128)
        want = (lane // 128) * stride + t - base
        inside = (t >= base) & (t < head_size)
        keep = ((src == want) & inside).astype(F32)
        first = (t >= PLAIN_HEAD_SIZE) & (t < PLAIN_HEAD_SIZE + half)
        second = (t >= PLAIN_HEAD_SIZE + half) & (t < head_size)
        swap = ((src == want - half) & second).astype(F32) - ((src == want + half) & first).astype(
            F32
        )
        a = dot(values, keep.astype(BF))
        b = dot(values, swap.astype(BF))
        cw = jnp.concatenate([cosine] * n_heads, axis=1)
        sw = jnp.concatenate([sine_part] * n_heads, axis=1)
        return (a * cw + b * sw).astype(BF)

    loads[0].wait()
    kv[z, x, :, 0 : heads * 128] = dot(normed_latent, upw[...]).astype(BF)
    kv[z, x, :, heads * 128 :] = turn(kr_ref[...], 1, PLAIN_HEAD_SIZE, D_ROPE)
    kz = [None]
    own = kv.at[z, x]
    for d in range(1, n_z):
        far = lax.rem(z + d, n_z)
        kz.append(send(own, own, kz_sem.at[d], (far * n_x + x, tp)))
    kx = [send(own, own, kx_sem.at[0], other_x)]
    qt[...] = turn(q_ref[...], heads, 0, head_size)

    for d in range(1, n_z):
        z_in[d].wait_recv()
        ref = xb.at[tp, block(d), x]
        x_in.append(send(ref, ref, x_sem.at[d], other_x))
        relay_tp(d, 0, x)
    for d in range(n_z):
        x_in[d].wait_recv()
        relay_tp(d, 1, ox)

    tile = 256
    inner = gate.shape[1]

    def accumulate(q, fresh):
        xin = xb[q].reshape(n_ep * cap, width)
        weight_rows = pl.ds(pl.multiple_of(q * width, width), width)

        def step(i, carry):
            cols = pl.ds(pl.multiple_of(i * tile, tile), tile)
            g = dot(xin, wg[weight_rows, cols])
            u = dot(xin, wu[weight_rows, cols])
            if fresh:
                gate[:, cols] = g
                up[:, cols] = u
            else:
                gate[:, cols] = gate[:, cols] + g
                up[:, cols] = up[:, cols] + u
            return carry

        lax.fori_loop(0, inner // tile, step, 0)

    loads[1].wait()
    loads[2].wait()
    accumulate(tp, True)
    for d in range(1, n_z):
        kz[d].wait_recv()
        ref = kv.at[block(d), x]
        kx.append(send(ref, ref, kx_sem.at[d], other_x))
    for cp in c_in:
        cp.wait_recv()
    accumulate(core, False)
    f_in = []
    for side, xi in ((0, x), (1, ox)):
        for d in range(n_z):
            y_in[side * n_z + d].wait_recv()
            ref = xb.at[over, block(d), xi]
            f_in.append(send(ref, ref, f_sem.at[d, side], to_core))
    accumulate(over, False)
    for cp in f_in:
        cp.wait_recv()

    q = diag
    xin = xb[q].reshape(n_ep * cap, width)
    weight_rows = pl.ds(pl.multiple_of(q * width, width), width)

    def last(i, carry):
        cols = pl.ds(pl.multiple_of(i * tile, tile), tile)
        g = gate[:, cols] + dot(xin, wg[weight_rows, cols])
        u = up[:, cols] + dot(xin, wu[weight_rows, cols])
        hidden[:, cols] = (g / (1.0 + jnp.exp(-g)) * u).astype(BF)
        return carry

    lax.fori_loop(0, inner // tile, last, 0)

    loads[3].wait()
    piece = n_x * cap

    def down(q, put):
        def step(i, carry):
            block_rows = pl.ds(pl.multiple_of(i * piece, piece), piece)
            cols = pl.ds(pl.multiple_of(q * width, width), width)
            put(i, block_rows, dot(hidden[block_rows, :], wd[:, cols]).astype(BF))
            return carry

        lax.fori_loop(0, n_z, step, 0)

    def put_pa(i, block_rows, value):
        pa[i] = value

    down(diag, put_pa)
    a_in = send(pa, ra, p_sem.at[0], to_core)

    def put_pb(i, block_rows, value):
        pb[i] = value

    down(over, put_pb)
    a_in.wait_recv()
    b_in = []
    for d in range(1, n_z + 1):
        s = block(d % n_z)
        pb[s] = (pb[s].astype(F32) + ra[s].astype(F32)).astype(BF)
        b_in.append(send(pb.at[s], rb.at[s], rb_sem.at[d - 1], to_y))

    def put_pc(i, block_rows, value):
        pc[i] = value

    down(core, put_pc)
    c2 = send(pc, rc, p_sem.at[1], to_core)

    def put_po(i, block_rows, value):
        po[i] = value

    down(tp, put_po)

    for cp in kx:
        cp.wait_recv()
    keys_all = n_ep * rows
    tail = kv[:, :, :, heads * 128 :].reshape(keys_all, 128)
    lane = lax.broadcasted_iota(jnp.int32, (keys_all, 128), 1)
    q_seg = (ep * rows + lax.broadcasted_iota(jnp.int32, (rows, keys_all), 0)) // SEGMENT
    k_seg = lax.broadcasted_iota(jnp.int32, (rows, keys_all), 1) // SEGMENT
    allowed = q_seg >= k_seg
    scale_factor = head_size ** (-0.5)
    for h in range(heads):
        kv_h = kv[:, :, :, h * 128 : (h + 1) * 128].reshape(keys_all, 128)
        key_h = jnp.where(lane < PLAIN_HEAD_SIZE, kv_h, tail)
        scores = lax.dot_general(
            qt[:, h * 128 : (h + 1) * 128],
            key_h,
            (((1,), (1,)), ((), ())),
            preferred_element_type=F32,
        )
        scores = jnp.where(allowed, scores * scale_factor, -jnp.inf)
        weights = jnp.exp(scores - jnp.max(scores, axis=-1, keepdims=True))
        denominator = jnp.sum(weights, axis=-1, keepdims=True)
        done = dot(weights.astype(BF), kv_h) / denominator
        att[:, h * VALUE_HEAD_SIZE : (h + 1) * VALUE_HEAD_SIZE] = done[:, PLAIN_HEAD_SIZE:].astype(BF)
    loads[4].wait()
    share = rows // 4
    for j in range(4):
        cols = slice(j * width, (j + 1) * width)
        mpart[:, :, cols] = dot(att[...], wout[:, cols]).astype(BF).reshape(4, share, width)
    m_in = []
    for i, (q, dev) in enumerate(((core, to_core), (over, to_y), (diag, (ep, diag)))):
        m_in.append(send(mpart.at[q], mrecv.at[i], m_sem.at[i], dev))

    c2.wait_recv()
    r_in = []
    for d in range(1, n_z + 1):
        dd = d % n_z
        s = block(dd)
        b_in[d - 1].wait_recv()
        total = po[s].astype(F32) + rc[s].astype(F32) + rb[s].astype(F32)
        rsend[s] = total.astype(BF).reshape(n_x, cap, width)
        for side, xi in ((0, x), (1, ox)):
            if dd == 0 and side == 0:
                ret[x, z] = rsend[z, x]
            else:
                r_in.append(
                    send(rsend.at[s, xi], ret.at[x, z], ret_sem.at[dd, side], (s * n_x + xi, tp))
                )

    for cp in m_in:
        cp.wait_recv()
    mix = mpart[tp].astype(F32)
    for i in range(3):
        mix = mix + mrecv[i].astype(F32)
    mix_ref[...] = mix.astype(BF)

    glog = glog_ref[...]
    own_logit = jnp.sum(
        jnp.where(lax.broadcasted_iota(jnp.int32, glog.shape, 1) == group, glog, 0.0),
        axis=1,
        keepdims=True,
    )
    group_share = 1.0 / jnp.sum(jnp.exp(glog - own_logit), axis=1, keepdims=True)
    gap = ilog_ref[:, 0:1] - ilog_ref[:, 1:2]
    w0 = group_share / (1.0 + jnp.exp(-gap))
    w1 = group_share / (1.0 + jnp.exp(gap))

    for cp in r_in:
        cp.wait_recv()
    table_b = table.astype(BF)
    total = jnp.zeros((rows, width), F32)
    for xi in range(n_x):
        wx = jnp.where(lax.rem(pick0, n_x) == xi, w0, 0.0) + jnp.where(
            lax.rem(pick1, n_x) == xi, w1, 0.0
        )
        total = total + wx * dot(table_b, ret[xi].reshape(n_z * cap, width))
    exp_ref[...] = total.astype(BF)
    for cp in pending:
        cp.wait_send()


def fused_device(n_z, n_x, *args):
    (q, lat, kr, lgain, upw, wout, tok, mgain, glog, ilog, pick, wg, wu, wd) = args
    rows = tok.shape[0]
    model = tok.shape[1]
    n_ep = n_z * n_x
    cap = 4 * rows // n_ep
    width = model // 4
    inner = wg.shape[2]
    heads = wout.shape[0] // VALUE_HEAD_SIZE
    slots = n_ep * cap
    lane = jnp.arange(128, dtype=jnp.int32)
    half = D_ROPE // 2
    j = (lane - PLAIN_HEAD_SIZE) % half
    frequency = jnp.power(10000.0, -j.astype(F32) * 2.0 / D_ROPE)
    positions = (lax.axis_index("ep") * rows + jnp.arange(rows, dtype=jnp.int32)).astype(F32)
    angles = positions[:, None] * frequency[None, :]
    turned = (lane >= PLAIN_HEAD_SIZE)[None, :]
    cosine = jnp.where(turned, jnp.cos(angles), 1.0)
    sine_part = jnp.where(turned, jnp.sin(angles), 0.0)
    dma = pltpu.SemaphoreType.DMA
    vmem = pltpu.VMEM
    spec_v = pl.BlockSpec(memory_space=pltpu.VMEM)
    spec_a = pl.BlockSpec(memory_space=pl.ANY)
    return pl.pallas_call(
        functools.partial(fused_kernel, n_z, n_x),
        out_shape=(
            jax.ShapeDtypeStruct((rows // 4, model), BF),
            jax.ShapeDtypeStruct((rows, width), BF),
        ),
        in_specs=[spec_v] * 11 + [spec_a] * 5,
        out_specs=(spec_v, spec_v),
        scratch_shapes=[
            vmem(upw.shape, BF),
            vmem(wout.shape, BF),
            vmem(wg.shape[1:], BF),
            vmem(wu.shape[1:], BF),
            vmem(wd.shape[1:], BF),
            vmem((rows, model), BF),
            vmem((n_z, cap, width), BF),
            vmem((4, n_z, n_x, cap, width), BF),
            vmem((slots, inner), F32),
            vmem((slots, inner), F32),
            vmem((slots, inner), BF),
        ]
        + [vmem((n_z, n_x * cap, width), BF)] * 7
        + [
            vmem((n_z, n_x, cap, width), BF),
            vmem((n_x, n_z, cap, width), BF),
            vmem((n_z, n_x, rows, heads * 128 + 128), BF),
            vmem((rows, heads * 128), BF),
            vmem((rows, heads * VALUE_HEAD_SIZE), BF),
            vmem((4, rows // 4, model), BF),
            vmem((3, rows // 4, model), BF),
            dma((5,)),
            dma((n_z, 2)),
            dma((n_z, 2)),
            dma((n_z, 2, 2)),
            dma((n_z, 2, 2)),
            dma((n_z, 2, 2)),
            dma((2, 2)),
            dma((n_z, 2)),
            dma((n_z, 2, 2)),
            dma((n_z, 2)),
            dma((n_z, 2)),
            dma((3, 2)),
        ],
        compiler_params=pltpu.CompilerParams(
            collective_id=0, has_side_effects=True, vmem_limit_bytes=60 * 1024 * 1024
        ),
    )(
        q,
        lat,
        kr,
        lgain.reshape(1, -1),
        tok,
        mgain.reshape(1, -1),
        glog,
        ilog,
        pick,
        cosine,
        sine_part,
        upw,
        wout,
        wg,
        wu,
        wd,
    )


def solution(mesh):
    n_ep = mesh.shape["ep"]
    n_tp = mesh.shape["tp"]

    def step(*args):
        groups = args[8].shape[1]
        if n_ep == 2 * groups and n_tp == 4:
            return fused_device(groups, 2, *args)
        return per_device(*args)

    in_specs = (
        P("ep", "tp"),
        P("ep", None),
        P("ep", None),
        P(),
        P(None, "tp"),
        P("tp", None),
        P("ep", None),
        P(),
        P("ep", None),
        P("ep", None),
        P("ep", None),
        P("ep", None, "tp"),
        P("ep", None, "tp"),
        P("ep", "tp", None),
    )
    out_specs = (P(("ep", "tp"), None), P("ep", "tp"))
    return jax.shard_map(
        step, mesh=mesh, in_specs=in_specs, out_specs=out_specs, check_vma=False
    )
```

```python
import functools

import jax
import jax.numpy as jnp
from jax import lax
from jax.experimental import pallas as pl
from jax.experimental.pallas import tpu as pltpu
from jax.sharding import PartitionSpec as P

PLAIN_HEAD_SIZE = 64
D_ROPE = 32
VALUE_HEAD_SIZE = 64
SEGMENT = 64


def rotate(values, positions):
    half_size = values.shape[-1] // 2
    frequency = jnp.power(
        10000.0, -jnp.arange(half_size, dtype=jnp.float32) * 2.0 / values.shape[-1]
    )
    angles = positions[:, None] * frequency[None, :]
    if values.ndim == 3:
        angles = angles[:, None, :]
    cosine = jnp.cos(angles)
    sine_part = jnp.sin(angles)
    first_half = values[..., :half_size]
    second_half = values[..., half_size:]
    return jnp.concatenate(
        [
            first_half * cosine - second_half * sine_part,
            second_half * cosine + first_half * sine_part,
        ],
        axis=-1,
    )


def finish_expert(gate_proj, up_proj, w_down, source_count, item_count, model_width):
    hidden = (jax.nn.silu(gate_proj) * up_proj).astype(jnp.bfloat16)
    partial_value = jnp.dot(hidden, w_down[0], preferred_element_type=jnp.float32)
    partial_value = partial_value.reshape(source_count, item_count, model_width)
    return lax.psum_scatter(
        partial_value.astype(jnp.bfloat16), "tp", scatter_dimension=2, tiled=True
    )


def per_device(
    queries,
    token_latents,
    key_rotary,
    latent_norm_gain,
    latent_up_weight,
    w_out,
    tokens_b,
    moe_gain,
    group_logits,
    inner_logits,
    expert_pick,
    w_gate,
    w_up,
    w_down,
):
    row_count = queries.shape[0]
    heads_here = w_out.shape[0] // VALUE_HEAD_SIZE
    offset = lax.axis_index("ep") * row_count
    token_index = offset + jnp.arange(row_count, dtype=jnp.int32)
    positions = token_index.astype(jnp.float32)
    query_heads = queries.reshape(row_count, heads_here, PLAIN_HEAD_SIZE + D_ROPE)
    q_plain = jnp.transpose(query_heads[:, :, :PLAIN_HEAD_SIZE], (1, 0, 2))
    q_turned = rotate(query_heads[:, :, PLAIN_HEAD_SIZE:].astype(jnp.float32), positions).astype(
        jnp.bfloat16
    )
    q_turned = jnp.transpose(q_turned, (1, 0, 2))
    latent = token_latents.astype(jnp.float32)
    normed_latent = (
        latent
        * lax.rsqrt(jnp.mean(latent * latent, axis=-1, keepdims=True) + 1e-06)
        * latent_norm_gain
    ).astype(jnp.bfloat16)
    k_turned = rotate(key_rotary.astype(jnp.float32), positions).astype(jnp.bfloat16)
    query_segment = token_index // SEGMENT
    scale_factor = (PLAIN_HEAD_SIZE + D_ROPE) ** (-0.5)
    own_keys = jnp.dot(normed_latent, latent_up_weight, preferred_element_type=jnp.float32).astype(
        jnp.bfloat16
    )
    shard_part = (
        lax.all_gather(own_keys, "ep", axis=0, tiled=True),
        lax.all_gather(k_turned, "ep", axis=0, tiled=True),
    )
    projected = shard_part[0].reshape(
        shard_part[0].shape[0], heads_here, PLAIN_HEAD_SIZE + VALUE_HEAD_SIZE
    )
    kv_heads = jnp.transpose(projected, (1, 0, 2))
    run_max = jnp.full((heads_here, row_count), -1e30, jnp.float32)
    key_count = kv_heads.shape[1]
    k_plain = kv_heads[:, :, :PLAIN_HEAD_SIZE]
    values = kv_heads[:, :, PLAIN_HEAD_SIZE:]
    scores = jnp.einsum("hqd,hkd->hqk", q_plain, k_plain, preferred_element_type=jnp.float32)
    scores = scores + jnp.einsum(
        "hqd,kd->hqk", q_turned, shard_part[1], preferred_element_type=jnp.float32
    )
    scores = scores * scale_factor
    key_segment = jnp.arange(key_count, dtype=jnp.int32) // SEGMENT
    allowed = query_segment[:, None] >= key_segment[None, :]
    scores = jnp.where(allowed[None], scores, -jnp.inf)
    new_max = jnp.maximum(run_max, jnp.max(scores, axis=-1))
    weights_raw = jnp.exp(scores - new_max[:, :, None])
    denominator = jnp.sum(weights_raw, axis=-1)
    update = jnp.einsum(
        "hqk,hkd->hqd", weights_raw.astype(jnp.bfloat16), values, preferred_element_type=jnp.float32
    )
    finished = (new_max, denominator, update)
    denominator = finished[1]
    attended = (finished[2] / denominator[:, :, None]).astype(jnp.bfloat16)
    attended = jnp.transpose(attended, (1, 0, 2)).reshape(row_count, heads_here * VALUE_HEAD_SIZE)
    mixer_out = lax.psum_scatter(
        jnp.dot(attended, w_out, preferred_element_type=jnp.float32).astype(jnp.bfloat16),
        "tp",
        scatter_dimension=0,
        tiled=True,
    )
    row_total = tokens_b.shape[0]
    model_width = tokens_b.shape[1]
    experts = lax.axis_size("ep")
    capacity = 4 * row_total // experts
    values_f = tokens_b.astype(jnp.float32)
    centered = values_f - jnp.mean(values_f, axis=-1, keepdims=True)
    variance = jnp.mean(centered * centered, axis=-1, keepdims=True)
    normed = (centered * lax.rsqrt(variance + 1e-05) * moe_gain).astype(jnp.bfloat16)
    flat_picks = expert_pick.reshape(-1)
    owner_row = jnp.arange(2 * row_total, dtype=jnp.int32) // 2
    hit_table = (flat_picks[:, None] == jnp.arange(experts, dtype=jnp.int32)[None, :]).astype(
        jnp.int32
    )
    order_in = jnp.sum(jnp.cumsum(hit_table, axis=0) * hit_table, axis=1) - 1
    slot_index = flat_picks * capacity + order_in
    slot_rows = jnp.zeros((experts * capacity,), jnp.int32).at[slot_index].set(owner_row)
    slot_filled = jnp.zeros((experts * capacity,), jnp.bfloat16).at[slot_index].set(1.0)
    outbound = (normed[slot_rows] * slot_filled[:, None]).reshape(experts, capacity, model_width)
    arrived = lax.all_to_all(outbound, "ep", split_axis=0, concat_axis=0, tiled=True)
    source_count = arrived.shape[0]
    item_count = arrived.shape[1]
    flat_rows = arrived.reshape(source_count * item_count, model_width)
    gate_proj = jnp.dot(flat_rows, w_gate[0], preferred_element_type=jnp.float32)
    up_proj = jnp.dot(flat_rows, w_up[0], preferred_element_type=jnp.float32)
    computed = finish_expert(gate_proj, up_proj, w_down, source_count, item_count, model_width)
    returned = lax.all_to_all(computed, "ep", split_axis=0, concat_axis=0, tiled=True)
    flat_back = returned.reshape(experts * capacity, returned.shape[2])
    chosen = flat_back[slot_index].astype(jnp.float32).reshape(row_total, 2, returned.shape[2])
    per_group = experts // group_logits.shape[1]
    home_group = expert_pick[:, 0] // per_group
    own_logit = jnp.sum(
        jnp.where(
            jnp.arange(group_logits.shape[1], dtype=jnp.int32)[None, :] == home_group[:, None],
            group_logits,
            0.0,
        ),
        axis=1,
    )
    group_share = 1.0 / jnp.sum(jnp.exp(group_logits - own_logit[:, None]), axis=1)
    logit_gap = inner_logits[:, 0] - inner_logits[:, 1]
    route_weight = group_share[:, None] * jnp.stack(
        [jax.nn.sigmoid(logit_gap), jax.nn.sigmoid(-logit_gap)], axis=1
    )
    expert_out = jnp.sum(route_weight[:, :, None] * chosen, axis=1).astype(jnp.bfloat16)
    return (mixer_out, expert_out)


MESH = pl.DeviceIdType.MESH
BF = jnp.bfloat16
F32 = jnp.float32


def dot(a, b):
    return jnp.dot(a, b, preferred_element_type=F32)


def fused_kernel(
    n_z,
    n_x,
    q_ref,
    lat_ref,
    kr_ref,
    lgain_ref,
    tok_ref,
    mgain_ref,
    glog_ref,
    ilog_ref,
    pick_ref,
    cos_ref,
    sin_ref,
    upw_hbm,
    wout_hbm,
    wg_hbm,
    wu_hbm,
    wd_hbm,
    mix_ref,
    exp_ref,
    upw,
    wout,
    wg,
    wu,
    wd,
    nrm,
    dsend,
    xb,
    gate,
    up,
    hidden,
    pa,
    ra,
    pb,
    rb,
    pc,
    rc,
    po,
    rsend,
    ret,
    kv,
    qt,
    att,
    mpart,
    mrecv,
    w_sem,
    z_sem,
    x_sem,
    y_sem,
    c_sem,
    f_sem,
    p_sem,
    rb_sem,
    ret_sem,
    kz_sem,
    kx_sem,
    m_sem,
    a_sem,
    narrow,
    mpair,
):
    ep = lax.axis_index("ep")
    tp = lax.axis_index("tp")
    z, x = ep // n_x, lax.rem(ep, n_x)
    y, c = tp // 2, lax.rem(tp, 2)
    ox = 1 - x
    rows = tok_ref.shape[0]
    cap = dsend.shape[1]
    width = dsend.shape[2]
    heads = qt.shape[1] // 128
    other_x = (z * n_x + ox, tp)
    core = tp + 1 - 2 * c
    over = tp + 2 - 4 * y
    diag = 3 - tp
    to_core, to_y = (ep, core), (ep, over)

    loads = []
    for i, (a, b) in enumerate(
        ((upw_hbm, upw), (wg_hbm.at[0], wg), (wu_hbm.at[0], wu), (wd_hbm.at[0], wd), (wout_hbm, wout))
    ):
        cp = pltpu.make_async_copy(a, b, w_sem.at[i])
        cp.start()
        loads.append(cp)

    barrier = pltpu.get_barrier_semaphore()
    n_ep = n_z * n_x
    for d in range(1, n_ep):
        pl.semaphore_signal(
            barrier, inc=1, device_id=(lax.rem(ep + d, n_ep), tp), device_id_type=MESH
        )
    for d in range(1, 4):
        pl.semaphore_signal(
            barrier, inc=1, device_id=(ep, lax.rem(tp + d, 4)), device_id_type=MESH
        )

    pending = []

    def send(src, dst, sem, device):
        cp = pltpu.make_async_remote_copy(
            src_ref=src,
            dst_ref=dst,
            send_sem=sem.at[0],
            recv_sem=sem.at[1],
            device_id=device,
            device_id_type=MESH,
        )
        cp.start()
        pending.append(cp)
        return cp

    values_f = tok_ref[...].astype(F32)
    centered = values_f - jnp.mean(values_f, axis=-1, keepdims=True)
    variance = jnp.mean(centered * centered, axis=-1, keepdims=True)
    nrm[...] = (centered * lax.rsqrt(variance + 1e-05) * mgain_ref[...]).astype(BF)
    mine = nrm[:, pl.ds(pl.multiple_of(tp * width, width), width)]
    narrow[...] = jnp.zeros_like(narrow)
    n_groups = glog_ref.shape[0]
    narrow[0:2, :] = pick_ref[...].astype(F32)
    narrow[8:10, :] = ilog_ref[...]
    narrow[16 : 16 + n_groups, :] = glog_ref[...]
    narrow[32 : 32 + D_ROPE, :] = kr_ref[...].astype(F32)
    tall = narrow[...].T
    pick0 = tall[:, 0:1].astype(jnp.int32)
    pick1 = tall[:, 1:2].astype(jnp.int32)
    group = pick0 // n_x
    group_one = (lax.broadcasted_iota(jnp.int32, (rows, 128), 1) == group).astype(F32)
    below = (
        lax.broadcasted_iota(jnp.int32, (rows, rows), 0)
        > lax.broadcasted_iota(jnp.int32, (rows, rows), 1)
    ).astype(F32)
    counts = dot(below.astype(BF), group_one.astype(BF))
    order_in = jnp.sum(counts * group_one, axis=1, keepdims=True)
    slot = group.astype(F32) * float(cap) + order_in
    slot_iota = lax.broadcasted_iota(jnp.int32, (rows, n_z * cap), 1).astype(F32)
    table = (slot_iota == slot).astype(F32)
    picked = dot(table.T.astype(BF), mine).astype(BF)
    dsend[...] = picked.reshape(n_z, cap, width)
    table_t = table.T.astype(BF)
    own_slots = (
        lax.broadcasted_iota(jnp.int32, (cap, n_z * cap), 0) + z * cap
        == lax.broadcasted_iota(jnp.int32, (cap, n_z * cap), 1)
    ).astype(F32).astype(BF)
    own_table = dot(own_slots, table_t).astype(BF)
    own_rows = dot(own_table, nrm[...]).astype(BF)
    for j in range(4):
        xb[j, z, x] = own_rows[:, j * width : (j + 1) * width]

    pl.semaphore_wait(barrier, n_ep + 2)

    z_in = [None]
    for d in range(1, n_z):
        far = lax.rem(z + d, n_z)
        z_in.append(send(dsend.at[far], xb.at[tp, z, x], z_sem.at[d], (far * n_x + x, tp)))

    def block(d):
        return lax.rem(z + n_z - d, n_z)

    x_in, y_in, c_in = [], [], []

    def relay_tp(d, side, xi):
        ref = xb.at[tp, block(d), xi]
        y_in.append(send(ref, ref, y_sem.at[d, side], to_y))
        c_in.append(send(ref, ref, c_sem.at[d, side], to_core))

    ref = xb.at[tp, z, x]
    x_in.append(send(dsend.at[z], ref, x_sem.at[0], other_x))

    latent = lat_ref[...].astype(F32)
    normed_latent = (
        latent
        * lax.rsqrt(jnp.mean(latent * latent, axis=-1, keepdims=True) + 1e-06)
        * lgain_ref[...]
    ).astype(BF)
    cosine, sine_part = cos_ref[...], sin_ref[...]
    half = D_ROPE // 2
    head_size = PLAIN_HEAD_SIZE + D_ROPE

    def turn(values, n_heads, base, stride):
        wide = n_heads * 128
        src = lax.broadcasted_iota(jnp.int32, (values.shape[1], wide), 0)
        lane = lax.broadcasted_iota(jnp.int32, (values.shape[1], wide), 1)
        t = lax.rem(lane, 128)
        want = (lane // 128) * stride + t - base
        inside = (t >= base) & (t < head_size)
        keep = ((src == want) & inside).astype(F32)
        first = (t >= PLAIN_HEAD_SIZE) & (t < PLAIN_HEAD_SIZE + half)
        second = (t >= PLAIN_HEAD_SIZE + half) & (t < head_size)
        swap = ((src == want - half) & second).astype(F32) - ((src == want + half) & first).astype(
            F32
        )
        a = dot(values, keep.astype(BF))
        b = dot(values, swap.astype(BF))
        cw = jnp.concatenate([cosine] * n_heads, axis=1)
        sw = jnp.concatenate([sine_part] * n_heads, axis=1)
        return (a * cw + b * sw).astype(BF)

    loads[0].wait()
    kv[z, x, :, 0 : heads * 128] = dot(normed_latent, upw[...]).astype(BF)
    kv[z, x, :, heads * 128 :] = turn(tall[:, 32 : 32 + D_ROPE].astype(BF), 1, PLAIN_HEAD_SIZE, D_ROPE)
    kz = [None]
    own = kv.at[z, x]
    for d in range(1, n_z):
        far = lax.rem(z + d, n_z)
        kz.append(send(own, own, kz_sem.at[d], (far * n_x + x, tp)))
    kx = []
    qt[...] = turn(q_ref[...], heads, 0, head_size)

    for d in range(1, n_z):
        z_in[d].wait_recv()
        ref = xb.at[tp, block(d), x]
        x_in.append(send(ref, ref, x_sem.at[d], other_x))
        relay_tp(d, 0, x)
    for d in range(n_z):
        x_in[d].wait_recv()
        relay_tp(d, 1, ox)

    kx.append(send(own, own, kx_sem.at[0], other_x))

    tile = 256
    inner = gate.shape[1]

    def accumulate(q, fresh):
        xin = xb[q].reshape(n_ep * cap, width)
        weight_rows = pl.ds(pl.multiple_of(q * width, width), width)

        def step(i, carry):
            cols = pl.ds(pl.multiple_of(i * tile, tile), tile)
            g = dot(xin, wg[weight_rows, cols])
            u = dot(xin, wu[weight_rows, cols])
            if fresh:
                gate[:, cols] = g
                up[:, cols] = u
            else:
                gate[:, cols] = gate[:, cols] + g
                up[:, cols] = up[:, cols] + u
            return carry

        lax.fori_loop(0, inner // tile, step, 0)

    loads[1].wait()
    loads[2].wait()
    accumulate(tp, True)
    for d in range(1, n_z):
        kz[d].wait_recv()
        ref = kv.at[block(d), x]
        kx.append(send(ref, ref, kx_sem.at[d], other_x))
    for cp in c_in:
        cp.wait_recv()
    accumulate(core, False)
    f_in = []
    stops = [(d, 0, x) for d in range(1, n_z)] + [(d, 1, ox) for d in range(n_z)]
    for arrival, (d, side, xi) in zip(y_in, stops):
        arrival.wait_recv()
        ref = xb.at[over, block(d), xi]
        f_in.append(send(ref, ref, f_sem.at[d, side], to_core))
    accumulate(over, False)
    for cp in f_in:
        cp.wait_recv()

    q = diag
    xin = xb[q].reshape(n_ep * cap, width)
    weight_rows = pl.ds(pl.multiple_of(q * width, width), width)

    def last(i, carry):
        cols = pl.ds(pl.multiple_of(i * tile, tile), tile)
        g = gate[:, cols] + dot(xin, wg[weight_rows, cols])
        u = up[:, cols] + dot(xin, wu[weight_rows, cols])
        hidden[:, cols] = (g / (1.0 + jnp.exp(-g)) * u).astype(BF)
        return carry

    lax.fori_loop(0, inner // tile, last, 0)

    loads[3].wait()
    piece = n_x * cap

    def down(q, put):
        def step(i, carry):
            block_rows = pl.ds(pl.multiple_of(i * piece, piece), piece)
            cols = pl.ds(pl.multiple_of(q * width, width), width)
            put(i, block_rows, dot(hidden[block_rows, :], wd[:, cols]).astype(BF))
            return carry

        lax.fori_loop(0, n_z, step, 0)

    def part(q, s):
        cols = pl.ds(pl.multiple_of(q * width, width), width)
        block_rows = pl.ds(pl.multiple_of(s * piece, piece), piece)
        return dot(hidden[block_rows, :], wd[:, cols]).astype(BF)

    a_in, b_in = [], []

    def pass_on(d):
        s = block(d % n_z)
        a_in[d - 1].wait_recv()
        pb[s] = (pb[s].astype(F32) + ra[s].astype(F32)).astype(BF)
        b_in.append(send(pb.at[s], rb.at[s], rb_sem.at[d - 1], to_y))

    for d in range(1, n_z + 1):
        s = block(d % n_z)
        pa[s] = part(diag, s)
        a_in.append(send(pa.at[s], ra.at[s], a_sem.at[d - 1], to_core))
        pb[s] = part(over, s)
        if d > 1:
            pass_on(d - 1)
    pass_on(n_z)

    def put_pc(i, block_rows, value):
        pc[i] = value

    down(core, put_pc)
    c2 = send(pc, rc, p_sem.at[1], to_core)

    def put_po(i, block_rows, value):
        po[i] = value

    down(tp, put_po)

    for cp in kx:
        cp.wait_recv()
    keys_all = n_ep * rows
    tail = kv[:, :, :, heads * 128 :].reshape(keys_all, 128)
    lane = lax.broadcasted_iota(jnp.int32, (keys_all, 128), 1)
    q_seg = (ep * rows + lax.broadcasted_iota(jnp.int32, (rows, keys_all), 0)) // SEGMENT
    k_seg = lax.broadcasted_iota(jnp.int32, (rows, keys_all), 1) // SEGMENT
    allowed = q_seg >= k_seg
    scale_factor = head_size ** (-0.5)
    for h in range(heads):
        kv_h = kv[:, :, :, h * 128 : (h + 1) * 128].reshape(keys_all, 128)
        key_h = jnp.where(lane < PLAIN_HEAD_SIZE, kv_h, tail)
        scores = lax.dot_general(
            qt[:, h * 128 : (h + 1) * 128],
            key_h,
            (((1,), (1,)), ((), ())),
            preferred_element_type=F32,
        )
        scores = jnp.where(allowed, scores * scale_factor, -jnp.inf)
        weights = jnp.exp(scores - jnp.max(scores, axis=-1, keepdims=True))
        denominator = jnp.sum(weights, axis=-1, keepdims=True)
        done = dot(weights.astype(BF), kv_h) / denominator
        att[:, h * VALUE_HEAD_SIZE : (h + 1) * VALUE_HEAD_SIZE] = done[:, PLAIN_HEAD_SIZE:].astype(BF)
    loads[4].wait()
    share = rows // 4
    for j in range(4):
        cols = slice(j * width, (j + 1) * width)
        mpart[:, :, cols] = dot(att[...], wout[:, cols]).astype(BF).reshape(4, share, width)
    m_in = []
    for i, q in enumerate((diag, core)):
        m_in.append(send(mpart.at[q], mrecv.at[i], m_sem.at[i], to_core))
    m_in[0].wait_recv()
    mpair[...] = (mpart[over].astype(F32) + mrecv[0].astype(F32)).astype(BF)
    m_in.append(send(mpair, mrecv.at[2], m_sem.at[2], to_y))

    c2.wait_recv()
    r_in = []
    for d in range(1, n_z + 1):
        dd = d % n_z
        s = block(dd)
        b_in[d - 1].wait_recv()
        total = po[s].astype(F32) + rc[s].astype(F32) + rb[s].astype(F32)
        rsend[s] = total.astype(BF).reshape(n_x, cap, width)
        for side, xi in ((0, x), (1, ox)):
            if dd == 0 and side == 0:
                ret[x, z] = rsend[z, x]
            else:
                r_in.append(
                    send(rsend.at[s, xi], ret.at[x, z], ret_sem.at[dd, side], (s * n_x + xi, tp))
                )

    for cp in m_in[1:]:
        cp.wait_recv()
    mix = mpart[tp].astype(F32)
    for i in range(1, 3):
        mix = mix + mrecv[i].astype(F32)
    mix_ref[...] = mix.astype(BF)

    glog = tall[:, 16 : 16 + n_groups]
    own_logit = jnp.sum(
        jnp.where(lax.broadcasted_iota(jnp.int32, glog.shape, 1) == group, glog, 0.0),
        axis=1,
        keepdims=True,
    )
    group_share = 1.0 / jnp.sum(jnp.exp(glog - own_logit), axis=1, keepdims=True)
    gap = tall[:, 8:9] - tall[:, 9:10]
    w0 = group_share / (1.0 + jnp.exp(-gap))
    w1 = group_share / (1.0 + jnp.exp(gap))

    for cp in r_in:
        cp.wait_recv()
    table_b = table.astype(BF)
    total = jnp.zeros((rows, width), F32)
    for xi in range(n_x):
        wx = jnp.where(lax.rem(pick0, n_x) == xi, w0, 0.0) + jnp.where(
            lax.rem(pick1, n_x) == xi, w1, 0.0
        )
        total = total + wx * dot(table_b, ret[xi].reshape(n_z * cap, width))
    exp_ref[...] = total.astype(BF)
    for cp in pending:
        cp.wait_send()


def fused_device(n_z, n_x, *args):
    (q, lat, kr, lgain, upw, wout, tok, mgain, glog, ilog, pick, wg, wu, wd) = args
    rows = tok.shape[0]
    model = tok.shape[1]
    n_ep = n_z * n_x
    cap = 4 * rows // n_ep
    width = model // 4
    inner = wg.shape[2]
    heads = wout.shape[0] // VALUE_HEAD_SIZE
    slots = n_ep * cap
    lane = jnp.arange(128, dtype=jnp.int32)
    half = D_ROPE // 2
    j = (lane - PLAIN_HEAD_SIZE) % half
    frequency = jnp.power(10000.0, -j.astype(F32) * 2.0 / D_ROPE)
    positions = (lax.axis_index("ep") * rows + jnp.arange(rows, dtype=jnp.int32)).astype(F32)
    angles = positions[:, None] * frequency[None, :]
    turned = (lane >= PLAIN_HEAD_SIZE)[None, :]
    cosine = jnp.where(turned, jnp.cos(angles), 1.0)
    sine_part = jnp.where(turned, jnp.sin(angles), 0.0)
    dma = pltpu.SemaphoreType.DMA
    vmem = pltpu.VMEM
    spec_v = pl.BlockSpec(memory_space=pltpu.VMEM)
    spec_a = pl.BlockSpec(memory_space=pl.ANY)
    return pl.pallas_call(
        functools.partial(fused_kernel, n_z, n_x),
        out_shape=(
            jax.ShapeDtypeStruct((rows // 4, model), BF),
            jax.ShapeDtypeStruct((rows, width), BF),
        ),
        in_specs=[spec_v] * 11 + [spec_a] * 5,
        out_specs=(spec_v, spec_v),
        scratch_shapes=[
            vmem(upw.shape, BF),
            vmem(wout.shape, BF),
            vmem(wg.shape[1:], BF),
            vmem(wu.shape[1:], BF),
            vmem(wd.shape[1:], BF),
            vmem((rows, model), BF),
            vmem((n_z, cap, width), BF),
            vmem((4, n_z, n_x, cap, width), BF),
            vmem((slots, inner), F32),
            vmem((slots, inner), F32),
            vmem((slots, inner), BF),
        ]
        + [vmem((n_z, n_x * cap, width), BF)] * 7
        + [
            vmem((n_z, n_x, cap, width), BF),
            vmem((n_x, n_z, cap, width), BF),
            vmem((n_z, n_x, rows, heads * 128 + 128), BF),
            vmem((rows, heads * 128), BF),
            vmem((rows, heads * VALUE_HEAD_SIZE), BF),
            vmem((4, rows // 4, model), BF),
            vmem((3, rows // 4, model), BF),
            dma((5,)),
            dma((n_z, 2)),
            dma((n_z, 2)),
            dma((n_z, 2, 2)),
            dma((n_z, 2, 2)),
            dma((n_z, 2, 2)),
            dma((2, 2)),
            dma((n_z, 2)),
            dma((n_z, 2, 2)),
            dma((n_z, 2)),
            dma((n_z, 2)),
            dma((4, 2)),
            dma((n_z, 2)),
            vmem((128, rows), F32),
            vmem((rows // 4, model), BF),
        ],
        compiler_params=pltpu.CompilerParams(
            collective_id=0, has_side_effects=True, vmem_limit_bytes=60 * 1024 * 1024
        ),
    )(
        q,
        lat,
        kr.T,
        lgain.reshape(1, -1),
        tok,
        mgain.reshape(1, -1),
        glog.T,
        ilog.T,
        pick.T,
        cosine,
        sine_part,
        upw,
        wout,
        wg,
        wu,
        wd,
    )


def solution(mesh):
    n_ep = mesh.shape["ep"]
    n_tp = mesh.shape["tp"]

    def step(*args):
        groups = args[8].shape[1]
        if n_ep == 2 * groups and n_tp == 4:
            return fused_device(groups, 2, *args)
        return per_device(*args)

    in_specs = (
        P("ep", "tp"),
        P("ep", None),
        P("ep", None),
        P(),
        P(None, "tp"),
        P("tp", None),
        P("ep", None),
        P(),
        P("ep", None),
        P("ep", None),
        P("ep", None),
        P("ep", None, "tp"),
        P("ep", None, "tp"),
        P("ep", "tp", None),
    )
    out_specs = (P(("ep", "tp"), None), P("ep", "tp"))
    return jax.shard_map(
        step, mesh=mesh, in_specs=in_specs, out_specs=out_specs, check_vma=False
    )
```
